32 devices in a mesh: grp: 2 (over y), dp: 2 (over x), kv: 4 (over z), tp: 2 (over core).
Axes of the slice: x: 2, y: 2, z: 4, core: 2. Of those that a mesh axis runs over, the one named last changes fastest.
Arguments:
- queries: bfloat16 [4, 1024, 2048], P(('grp', 'dp'), 'kv', 'tp'), parts along dimension 0, may hold values from -10 to 10
- keys: bfloat16 [4, 1024, 512], P(('grp', 'dp'), 'kv', 'tp'), parts along dimension 0, may hold values from -10 to 10
- values: bfloat16 [4, 1024, 512], P(('grp', 'dp'), 'kv', 'tp'), parts along dimension 0, may hold values from -6 to 6
- gate_logits: float32 [4, 2, 1024, 32], P(('grp', 'dp'), None, 'kv', 'tp'), parts along dimension 0, may hold values from -6 to 6
- chosen: int32 [4, 8, 8, 16], P(('grp', 'dp'), 'kv', 'tp'), parts along dimension 0, may hold values from -1 to 15, as said below
- pool_k: float32 [32, 64], replicated, may hold values from 0 to 0.35
- pool_v: float32 [32, 64], replicated, may hold values from 0 to 0.35
- out_gain: float32 [2048], P('tp'), may hold values from 0.1 to 1.9
Outputs:
- attended: bfloat16 [4, 1024, 2048], P(('grp', 'dp'), 'kv', 'tp'), parts along dimension 0
The draws below stay inside these ranges and needn't reach their ends.
There are 2 independent parts, one for each index of `grp`. The reference program is written for one: setup_inputs(seed, part) draws one part's arguments, and reference() takes and returns one part's arrays. A program takes and returns all parts, laid end to end along the dimension named above; an argument that names none is the same for every part. Nothing has to cross between parts.
Inputs may be any that keep to these rules, and one draw needn't show every extreme that they name: Entries are key block numbers (block e holds positions e * 64 to e * 64 + 63) or -1 for none. The list of query block b (positions b * 128 onward) holds the blocks that contain its own positions, other distinct blocks that begin before it, and -1 in its remaining entries. For the query blocks of one span of 256 positions and one key head, the blocks chosen from any other span number at most 2; in every draw some span reaches 2.
All inputs are finite; a program needn't handle non-finite values.
Results may differ from the reference program's by a relative error of at most 0.0079.
Values may be sent and summed in bfloat16 or wider, within the bound.
A program may use at most 64 MiB of HBM per device.

```python
import jax
import jax.numpy as jnp
from jax import lax

H = 32
G = 8
DH = 64
HPG = 4
CMP_STRIDE = 16
CMP_BLOCK = 32
SLC = 64
QB = 128
NSEL = 16
MOST = 2
TOK_DEV = 256
SEQS = 2
SEQLEN = 1024
N_KV = 4


def base_field(key, shape):
    return jnp.clip(jax.random.normal(key, shape, jnp.float32), -6.0, 6.0)


def draw_queries(key, part):
    field = base_field(jax.random.fold_in(key, 1), (SEQS, SEQLEN, H * DH))
    return field.astype(jnp.bfloat16)


def draw_keys(key, part):
    field = base_field(jax.random.fold_in(key, 2), (SEQS, SEQLEN, G * DH))
    return field.astype(jnp.bfloat16)


def draw_chosen(key, part):
    nqb = SEQLEN // QB
    per_owner = TOK_DEV // SLC
    total = SEQLEN // SLC
    own = QB // SLC
    per_span = TOK_DEV // QB
    base = jax.random.fold_in(key, 101)
    pop_key, set_key, pick_key = jax.random.split(base, 3)
    favour = jax.random.randint(pop_key, (SEQS, total), 0, 3)
    raw = jax.random.randint(set_key, (SEQS, N_KV, G, N_KV, per_owner), 0, 65536)
    setscore = (raw - favour.reshape(SEQS, 1, 1, N_KV, per_owner) * 40000) * per_owner + jnp.arange(per_owner)
    rank = jnp.sum(setscore[..., None, :] < setscore[..., :, None], axis=-1)
    inset = rank < MOST
    blocks = jnp.arange(nqb)
    span = blocks // per_span
    inset_q = inset[:, span].reshape(SEQS, nqb, G, total)
    number = jnp.arange(total)
    owner = number // per_owner
    remote = owner[None, :] < span[:, None]
    earlier = (owner[None, :] == span[:, None]) & (number[None, :] < blocks[:, None] * own)
    mine = number[None, :] // own == blocks[:, None]
    near = (owner[None, :] == span[:, None] - 1) | (owner[None, :] == span[:, None] - N_KV // 2) & (span[:, None] >= N_KV // 2)
    avail = remote[None, :, None, :] & inset_q | earlier[None, :, None, :]
    forced = mine[None, :, None, :] | (remote & near)[None, :, None, :] & inset_q
    noise = jax.random.randint(pick_key, (SEQS, nqb, G, total), 0, 65536) - favour[:, None, None, :] * 20000
    prio = jnp.where(forced, 0, jnp.where(avail, noise + 40001, 1 << 22))
    order = jnp.argsort(prio * total + number, axis=-1)[..., :NSEL]
    picked = jnp.take_along_axis(prio, order, axis=-1)
    return jnp.where(picked < 1 << 22, order, -1).astype(jnp.int32)


def levels(stream_key, dims, shards, smallest, largest):
    gain = 1.0
    for position, blocks in shards:
        draws = jax.random.uniform(jax.random.fold_in(jax.random.fold_in(stream_key, 6), position), (blocks,), jnp.float32, smallest / len(shards), largest / len(shards))
        gain = gain * jnp.repeat(jnp.exp(draws), dims[position] // blocks).reshape((-1,) + (1,) * (len(dims) - 1 - position))
    return gain


def normal_values(own_key, shape, deviation, most, cuts=(), held_as=jnp.bfloat16):
    result = deviation * jax.random.normal(own_key, shape, jnp.float32)
    if cuts:
        result = result * levels(own_key, shape, cuts, -0.22, 0.18)
    return jnp.clip(result, -most, most).astype(held_as)


def setup_inputs(seed: int = 0, part: int = 0) -> dict:
    streams_of = jax.random.split(jax.random.key(seed), 9)
    own_keys = jax.random.split(jax.random.fold_in(streams_of[8], part), 9)
    return {
        "queries": draw_queries(jax.random.fold_in(jax.random.fold_in(streams_of[8], part), 71), part),
        "keys": draw_keys(jax.random.fold_in(jax.random.fold_in(streams_of[8], part), 71), part),
        "values": normal_values(own_keys[2], (SEQS, SEQLEN, G * DH), 1.0, 6.0, ((0, 2), (1, 4), (2, 2))),
        "gate_logits": normal_values(own_keys[3], (SEQS, 2, SEQLEN, H), 1.5, 6.0, ((0, 2), (2, 4), (3, 2)), jnp.float32),
        "chosen": draw_chosen(jax.random.fold_in(jax.random.fold_in(streams_of[8], part), 71), part),
        "pool_k": jnp.clip(jax.random.uniform(streams_of[5], (CMP_BLOCK, DH), jnp.float32, 0.0, 0.35), 0.0, 0.35),
        "pool_v": jnp.clip(jax.random.uniform(streams_of[6], (CMP_BLOCK, DH), jnp.float32, 0.0, 0.35), 0.0, 0.35),
        "out_gain": jnp.clip(1.0 + 0.18 * jax.random.normal(streams_of[7], (H * DH,), jnp.float32), 0.1, 1.9),
    }


THETA = 500000.0
EPS = 1e-06
NEG = -1e+30

def rotate(matrix, start, heads):
    length = matrix.shape[0]
    half = DH // 2
    place = (start + jnp.arange(length)).astype(jnp.float32)
    freq = jnp.power(jnp.float32(THETA), -(2.0 * jnp.arange(half).astype(jnp.float32)) / DH)
    angle = place[:, None] * freq[None, :]
    cosine = jnp.cos(angle)[:, None, :]
    sine = jnp.sin(angle)[:, None, :]
    parts = matrix.reshape(length, heads, DH).astype(jnp.float32)
    first = parts[..., :half]
    second = parts[..., half:]
    turned = jnp.concatenate([first * cosine - second * sine, second * cosine + first * sine], -1)
    return turned.reshape(length, heads * DH).astype(jnp.bfloat16)

def compress(extended, pool, groups):
    count = extended.shape[0] // CMP_STRIDE - 1
    parts = extended.reshape(count + 1, CMP_STRIDE, groups, DH).astype(jnp.float32)
    lower = jnp.einsum('nigd,id->ngd', parts[:-1], pool[:CMP_STRIDE], precision=lax.Precision.HIGHEST)
    upper = jnp.einsum('nigd,id->ngd', parts[1:], pool[CMP_STRIDE:], precision=lax.Precision.HIGHEST)
    return (lower + upper).astype(jnp.bfloat16)

def reference(queries, keys, values, gate_logits, chosen, pool_k, pool_v, out_gain):
    scale = DH ** (-0.5)

    def one_sequence(item):
        query_seq, key_seq, value_seq, logits, lists = item
        length = query_seq.shape[0]
        query_turned = rotate(query_seq, 0, H)
        key_turned = rotate(key_seq, 0, G)
        padding = jnp.zeros((CMP_STRIDE, G * DH), key_seq.dtype)
        key_summary = compress(jnp.concatenate([key_seq, padding], 0), pool_k, G).astype(jnp.float32)
        value_summary = compress(jnp.concatenate([value_seq, padding], 0), pool_v, G).astype(jnp.float32)
        count = length // CMP_STRIDE
        ends = jnp.arange(count) * CMP_STRIDE + CMP_BLOCK - 1
        key_blocks = key_turned.reshape(length // SLC, SLC, G, DH)
        value_blocks = value_seq.reshape(length // SLC, SLC, G, DH)
        group_pick = jnp.arange(G)[:, None]

        def block(index):
            start = index * QB
            place = start + jnp.arange(QB)
            query_rows = lax.dynamic_slice_in_dim(query_seq, start, QB, 0).reshape(QB, G, HPG, DH).astype(jnp.float32)
            query_turn = lax.dynamic_slice_in_dim(query_turned, start, QB, 0).reshape(QB, G, HPG, DH).astype(jnp.float32)
            score = jnp.einsum('tghd,ngd->ghtn', query_rows, key_summary) * scale
            allow = (ends[None, :] <= place[:, None])[None, None]
            score = jnp.where(allow, score, NEG)
            top = lax.optimization_barrier(jnp.max(score, -1, keepdims=True))
            weight = jnp.where(allow, jnp.exp(score - top), 0.0)
            total = jnp.maximum(lax.optimization_barrier(jnp.sum(weight, -1)), 1.0)
            rounded = lax.optimization_barrier(weight.astype(jnp.bfloat16)).astype(jnp.float32)
            summary_out = jnp.einsum('ghtn,ngd->ghtd', rounded, value_summary) / total[..., None]
            picks = lists[index]
            safe = jnp.maximum(picks, 0)
            key_sel = key_blocks[safe, :, group_pick, :].astype(jnp.float32)
            value_sel = value_blocks[safe, :, group_pick, :].reshape(G, NSEL * SLC, DH).astype(jnp.float32)
            key_place = (safe[..., None] * SLC + jnp.arange(SLC)).reshape(G, NSEL * SLC)
            live = jnp.broadcast_to(picks[..., None] >= 0, (G, NSEL, SLC)).reshape(G, NSEL * SLC)
            allow_sel = (live[:, None, :] & (key_place[:, None, :] <= place[None, :, None]))[:, None]
            chosen_score = jnp.einsum('tghd,gnkd->ghtnk', query_turn, key_sel).reshape(G, HPG, QB, NSEL * SLC) * scale
            chosen_score = jnp.where(allow_sel, chosen_score, NEG)
            top_sel = lax.optimization_barrier(jnp.max(chosen_score, -1, keepdims=True))
            weight_sel = jnp.where(allow_sel, jnp.exp(chosen_score - top_sel), 0.0)
            total_sel = lax.optimization_barrier(jnp.sum(weight_sel, -1))
            rounded_sel = lax.optimization_barrier(weight_sel.astype(jnp.bfloat16)).astype(jnp.float32)
            chosen_out = jnp.einsum('ghtk,gkd->ghtd', rounded_sel, value_sel) / total_sel[..., None]
            gates = jax.nn.sigmoid(lax.dynamic_slice_in_dim(logits, start, QB, 1))
            gates = gates.reshape(2, QB, G, HPG).transpose(0, 2, 3, 1)
            mixed = gates[0][..., None] * summary_out + gates[1][..., None] * chosen_out
            mixed = mixed.transpose(2, 0, 1, 3).reshape(QB, H, DH)
            normed = mixed * lax.rsqrt(lax.optimization_barrier(jnp.mean(mixed * mixed, -1, keepdims=True)) + EPS) * out_gain.reshape(H, DH)
            return normed.reshape(QB, H * DH).astype(jnp.bfloat16)
        return lax.map(block, jnp.arange(length // QB)).reshape(length, H * DH)
    return lax.map(one_sequence, (queries, keys, values, gate_logits, chosen))
```

```python
import functools

import jax
import jax.numpy as jnp
from jax import lax
from jax.experimental import pallas as pl
from jax.experimental.pallas import tpu as pltpu
from jax.sharding import PartitionSpec as P

DH = 64
CMP_STRIDE = 16
CMP_BLOCK = 32
SLC = 64
QB = 128
MOST = 2
THETA = 500000.0
EPS = 1e-06
NEG = -1e30
LOG2E = 1.4426950408889634
MESH = pl.DeviceIdType.MESH


def rope_table(start, length):
    half = DH // 2
    lane = jnp.arange(2 * DH)
    freq = jnp.power(jnp.float32(THETA), -(2.0 * (lane % half).astype(jnp.float32)) / DH)
    angle = (start + jnp.arange(length)).astype(jnp.float32)[:, None] * freq[None, :]
    sign = jnp.where(lane % DH < half, -1.0, 1.0).astype(jnp.float32)
    return jnp.cos(angle), jnp.sin(angle) * sign[None, :]


def turn(x, cosine, sine):
    half = DH // 2
    lane = lax.broadcasted_iota(jnp.int32, x.shape, 1)
    partner = jnp.where(lane % DH < half, pltpu.roll(x, 2 * DH - half, 1), pltpu.roll(x, half, 1))
    return (x * cosine + partner * sine).astype(jnp.bfloat16)


def kernel(
    n, q_ref, k_ref, v_ref, gate_ref, list_ref, pk_ref, pv_ref, gain_ref, cos_ref, sin_ref,
    out_ref,
    qt, kt, vtl, kk, kkr, vtr, skk, svt, req, reqbuf, flag, own_bias, far_bias,
    sumbuf, edge, sendk, sendv, recvk, recvv, bias,
    top, total, acc, stot, sacc,
    req_send, req_recv, sum_send, sum_recv, edge_send, edge_recv,
    k_send, k_recv, v_send, v_recv,
):
    me = lax.axis_index("kv")
    length = q_ref.shape[1]
    heads = q_ref.shape[2] // DH
    groups = k_ref.shape[2] // DH
    per_group = heads // groups
    pairs = per_group // 2
    slabs = groups // 2
    qblocks = length // QB
    per = length // SLC
    count = length // CMP_STRIDE
    scale = DH ** (-0.5) * LOG2E
    f32 = jnp.float32

    barrier = pltpu.get_barrier_semaphore()
    for d in range(1, n):
        pl.semaphore_signal(
            barrier, inc=1, device_id={"kv": lax.rem(me + d, n)}, device_id_type=MESH
        )

    lanes = req.shape[1]
    rows = qblocks * groups

    def column(x, at):
        spot = lax.broadcasted_iota(jnp.int32, x.shape, 1) == at
        picked = jnp.sum(jnp.where(spot, x.astype(f32), 0.0), 1, keepdims=True)
        return jnp.broadcast_to(picked, (x.shape[0], QB))

    lists = jnp.concatenate([list_ref[0, b] for b in range(qblocks)], 0)
    lane = lax.broadcasted_iota(jnp.int32, (rows, lanes), 1)
    member = jnp.zeros((rows, lanes), jnp.int32)
    for i in range(lists.shape[1]):
        member = jnp.where(lists[:, i : i + 1] == lane, 1, member)
    union = member[:groups]
    for b in range(1, qblocks):
        union = jnp.maximum(union, member[b * groups : (b + 1) * groups])
    union = jnp.concatenate([union] * qblocks, 0)
    inner = lane % per
    rank = jnp.zeros_like(union)
    for d in range(1, per):
        rank = rank + jnp.where(inner >= d, pltpu.roll(union, d, 1), 0)

    def first_of(x):
        found = x
        for d in range(1, per):
            found = found + pltpu.roll(x, lanes - d, 1)
        return found

    for j in range(MOST):
        hit = (union == 1) & (rank == j)
        asked = first_of(jnp.where(hit, inner, 0))
        req[j * groups : (j + 1) * groups, :] = asked[:groups]
        flag[j * rows : (j + 1) * rows, :] = first_of(jnp.where(hit, member, 0))
    for i in range(per):
        own_bias[i] = jnp.where(column(member, me * per + i) > 0.5, 0.0, NEG)

    pl.semaphore_wait(barrier, n - 1)

    def remote(src, dst, send, recv, peer, origin):
        return pltpu.make_async_remote_copy(
            src_ref=src, dst_ref=dst, send_sem=send.at[peer], recv_sem=recv.at[origin],
            device_id={"kv": peer}, device_id_type=MESH,
        )

    def ask(peer, origin):
        return remote(req, reqbuf.at[origin], req_send, req_recv, peer, origin)

    def give_sum(peer, origin):
        return remote(sumbuf.at[origin], sumbuf.at[origin], sum_send, sum_recv, peer, origin)

    def give_edge(peer, origin):
        return remote(edge.at[origin], edge.at[origin], edge_send, edge_recv, peer, origin)

    def give_k(peer, origin):
        return remote(sendk.at[peer], recvk.at[origin], k_send, k_recv, peer, origin)

    def give_v(peer, origin):
        return remote(sendv.at[peer], recvv.at[origin], v_send, v_recv, peer, origin)

    @pl.loop(0, me)
    def _(d):
        ask(me - 1 - d, me).start()

    cosine = cos_ref[...]
    sine = sin_ref[...]
    low = lax.broadcasted_iota(jnp.int32, (length, 2 * DH), 1) < DH
    for p in range(slabs):
        cols = slice(p * 2 * DH, (p + 1) * 2 * DH)
        turned = turn(k_ref[0, :, cols].astype(f32), cosine, sine)
        kt[:, cols] = turned
    row = lax.broadcasted_iota(jnp.int32, (count, 2 * DH), 0)
    for w, (src, pool_ref) in enumerate(((k_ref, pk_ref), (v_ref, pv_ref))):
        pool = pool_ref[...]
        pool = jnp.concatenate([pool, pool], 1)
        for p in range(slabs):
            cols = slice(p * 2 * DH, (p + 1) * 2 * DH)
            x = src[0, :, cols].astype(f32).reshape(count, CMP_STRIDE, 2 * DH)
            lower = jnp.sum(x * pool[None, :CMP_STRIDE], 1)
            upper = jnp.sum(x * pool[None, CMP_STRIDE:], 1)
            following = jnp.where(row == count - 1, 0.0, pltpu.roll(upper, count - 1, 0))
            sumbuf[me, w, :, cols] = (lower + following).astype(jnp.bfloat16)
            edge[me, 2 * w : 2 * w + 1, cols] = lower[count - 1 :]
            edge[me, 2 * w + 1 : 2 * w + 2, cols] = upper[:1]

    @pl.loop(me + 1, n)
    def _(r):
        give_sum(r, me).start()
        give_edge(r, me).start()

    low_slc = lax.broadcasted_iota(jnp.int32, (SLC, 2 * DH), 1) < DH

    @pl.loop(me + 1, n)
    def _(r):
        ask(me, r).wait_recv()
        ids = column(reqbuf[r], me * per)
        for j in range(MOST):
            place = slice(j * SLC, (j + 1) * SLC)
            for p in range(slabs):
                cols = slice(p * 2 * DH, (p + 1) * 2 * DH)
                at = j * groups + 2 * p
                pick = jnp.where(low_slc, ids[at : at + 1], ids[at + 1 : at + 2])
                k_block = kt[:SLC, cols].astype(f32)
                v_block = v_ref[0, :SLC, cols].astype(f32)
                for i in range(1, per):
                    span = slice(i * SLC, (i + 1) * SLC)
                    match = pick > i - 0.5
                    k_block = jnp.where(match, kt[span, cols].astype(f32), k_block)
                    v_block = jnp.where(match, v_ref[0, span, cols].astype(f32), v_block)
                sendk[r, place, cols] = k_block.astype(jnp.bfloat16)
                sendv[r, place, cols] = v_block.astype(jnp.bfloat16)
        give_k(r, me).start()
        give_v(r, me).start()

    @pl.loop(0, heads // 2)
    def _(p):
        cols = pl.ds(pl.multiple_of(p * 2 * DH, 2 * DH), 2 * DH)
        qt[p] = turn(q_ref[0, :, cols].astype(f32), cosine, sine)

    def spread(slab, g, dst):
        keep = lax.broadcasted_iota(jnp.int32, slab.shape, 1) < DH
        wide = slab.astype(f32)
        swapped = pltpu.roll(wide, DH, 1)
        first, second = (wide, swapped) if g % 2 == 0 else (swapped, wide)
        dst[g, 0] = jnp.where(keep, first, 0.0).astype(jnp.bfloat16)
        dst[g, 1] = jnp.where(keep, 0.0, second).astype(jnp.bfloat16)

    def transposed(slab):
        return slab.astype(f32).T.astype(jnp.bfloat16)

    def score(keys, queries):
        return lax.dot_general(
            keys, queries, (((1,), (1,)), ((), ())), preferred_element_type=f32
        )

    for g in range(groups):
        spread(kt[:, (g // 2) * 2 * DH : (g // 2 + 1) * 2 * DH], g, kk)
    for p in range(slabs):
        flip = transposed(v_ref[0, :, p * 2 * DH : (p + 1) * 2 * DH])
        vtl[2 * p] = flip[:DH]
        vtl[2 * p + 1] = flip[DH:]
    key_at = lax.broadcasted_iota(jnp.int32, (SLC, QB), 0)
    token_at = lax.broadcasted_iota(jnp.int32, (SLC, QB), 1)

    @pl.loop(0, groups)
    def _(g):
        for b in range(qblocks):
            for i in range(per):
                value = own_bias[i, pl.ds(b * groups + g, 1), :]
                tile = jnp.where(key_at + i * SLC <= token_at + b * QB, value, NEG)
                bias[i * SLC : (i + 1) * SLC, b * QB : (b + 1) * QB] = tile
        for pair in range(pairs):
            queries = qt[g * pairs + pair]
            for e in range(2):
                h = g * per_group + 2 * pair + e
                s = score(kk[g, e], queries) * scale + bias[...]
                m = jnp.max(s, 0, keepdims=True)
                w = jnp.exp2(s - m)
                top[h] = m
                total[h] = jnp.sum(w, 0, keepdims=True)
                acc[h] = jnp.dot(vtl[g], w.astype(jnp.bfloat16), preferred_element_type=f32)

    @pl.loop(0, me)
    def _(d):
        give_sum(me, me - 1 - d).wait_recv()
        give_edge(me, me - 1 - d).wait_recv()

    for s in range(n):
        for w in range(2):
            place = slice(s * count, (s + 1) * count)
            for p in range(slabs):
                cols = slice(p * 2 * DH, (p + 1) * 2 * DH)
                following = edge[min(s + 1, n - 1), 2 * w + 1 : 2 * w + 2, cols]
                last = edge[s, 2 * w : 2 * w + 1, cols] + following
                own = sumbuf[s, w, :, cols].astype(f32)
                joined = jnp.where((row == count - 1) & (s < me), last, own)
                joined = jnp.where(s <= me, joined, 0.0)
                if w == 0:
                    for o in range(2):
                        lanes_low = lax.broadcasted_iota(jnp.int32, joined.shape, 1) < DH
                        swapped = pltpu.roll(joined, DH, 1)
                        first, second = (joined, swapped) if o == 0 else (swapped, joined)
                        skk[2 * p + o, 0, place] = jnp.where(lanes_low, first, 0.0).astype(
                            jnp.bfloat16
                        )
                        skk[2 * p + o, 1, place] = jnp.where(lanes_low, 0.0, second).astype(
                            jnp.bfloat16
                        )
                else:
                    svt[place, cols] = joined.astype(jnp.bfloat16)
    part_at = lax.broadcasted_iota(jnp.int32, (n * count, length), 0)
    time_at = lax.broadcasted_iota(jnp.int32, (n * count, length), 1) + me * length
    seen = part_at * CMP_STRIDE + CMP_BLOCK - 1 <= time_at
    sbias = jnp.where(seen, 0.0, NEG)
    flips = [transposed(svt[:, p * 2 * DH : (p + 1) * 2 * DH]) for p in range(slabs)]
    for g in range(groups):
        vt = flips[g // 2][(g % 2) * DH : (g % 2 + 1) * DH]
        for pair in range(pairs):
            queries = q_ref[0, :, (g * pairs + pair) * 2 * DH : (g * pairs + pair + 1) * 2 * DH]
            for e in range(2):
                h = g * per_group + 2 * pair + e
                s = score(skk[g, e], queries) * scale + sbias
                m = jnp.maximum(jnp.max(s, 0, keepdims=True), 0.1 * NEG)
                w = jnp.exp2(s - m)
                stot[h] = jnp.sum(w, 0, keepdims=True)
                sacc[h] = jnp.dot(vt, w.astype(jnp.bfloat16), preferred_element_type=f32)

    @pl.loop(0, me)
    def _(d):
        s = me - 1 - d
        give_k(me, s).wait_recv()
        give_v(me, s).wait_recv()
        far_bias[...] = jnp.where(column(flag[...], s * per) > 0.5, 0.0, NEG)
        for g in range(groups):
            spread(recvk[s, :, (g // 2) * 2 * DH : (g // 2 + 1) * 2 * DH], g, kkr)
        for p in range(slabs):
            flip = transposed(recvv[s, :, p * 2 * DH : (p + 1) * 2 * DH])
            vtr[2 * p] = flip[:DH]
            vtr[2 * p + 1] = flip[DH:]

        @pl.loop(0, groups)
        def _(g):
            rowed = [
                jnp.concatenate(
                    [
                        far_bias[pl.ds((j * qblocks + b) * groups + g, 1), :]
                        for b in range(qblocks)
                    ],
                    1,
                )
                for j in range(MOST)
            ]
            for pair in range(pairs):
                queries = qt[g * pairs + pair]
                for e in range(2):
                    h = g * per_group + 2 * pair + e
                    raw = score(kkr[g, e], queries) * scale
                    sc = jnp.concatenate(
                        [raw[j * SLC : (j + 1) * SLC] + rowed[j] for j in range(MOST)], 0
                    )
                    old = top[h]
                    m = jnp.maximum(jnp.max(sc, 0, keepdims=True), old)
                    w = jnp.exp2(sc - m)
                    shrink = jnp.exp2(old - m)
                    top[h] = m
                    total[h] = total[h] * shrink + jnp.sum(w, 0, keepdims=True)
                    acc[h] = acc[h] * shrink + jnp.dot(
                        vtr[g], w.astype(jnp.bfloat16), preferred_element_type=f32
                    )

    for pair in range(heads // 2):
        both = []
        for e in range(2):
            h = 2 * pair + e
            mixed = sacc[h] * (gate_ref[0, h : h + 1] / jnp.maximum(stot[h], 1.0)) + acc[h] * (
                gate_ref[1, h : h + 1] / total[h]
            )
            mean = jnp.sum(mixed * mixed, 0, keepdims=True) * (1.0 / DH)
            both.append(mixed * lax.rsqrt(mean + EPS))
        cols = slice(pair * 2 * DH, (pair + 1) * 2 * DH)
        flat = jnp.concatenate(both, 0).T
        out_ref[0, :, cols] = (flat * gain_ref[:, cols]).astype(jnp.bfloat16)

    @pl.loop(0, me)
    def _(d):
        ask(me - 1 - d, me).wait_send()

    @pl.loop(me + 1, n)
    def _(r):
        give_sum(r, me).wait_send()
        give_edge(r, me).wait_send()
        give_k(r, me).wait_send()
        give_v(r, me).wait_send()


def per_device(queries, keys, values, gate_logits, chosen, pool_k, pool_v, out_gain):
    n = lax.axis_size("kv")
    length = queries.shape[1]
    groups = keys.shape[2] // DH
    heads = queries.shape[2] // DH
    qblocks = length // QB
    count = length // CMP_STRIDE
    total = n * (length // SLC)
    lanes = -(-total // 128) * 128
    rows = qblocks * groups
    width = groups * DH
    cosine, sine = rope_table(lax.axis_index("kv") * length, length)
    gates = jax.nn.sigmoid(gate_logits[0]).transpose(0, 2, 1)
    bf16, f32, i32 = jnp.bfloat16, jnp.float32, jnp.int32
    vm, dma = pltpu.VMEM, pltpu.SemaphoreType.DMA
    scratch = [
        vm((heads // 2, length, 2 * DH), bf16),
        vm((length, width), bf16),
        vm((groups, DH, length), bf16),
        vm((groups, 2, length, 2 * DH), bf16),
        vm((groups, 2, MOST * SLC, 2 * DH), bf16),
        vm((groups, DH, MOST * SLC), bf16),
        vm((groups, 2, n * count, 2 * DH), bf16),
        vm((n * count, width), bf16),
        vm((MOST * groups, lanes), i32),
        vm((n, MOST * groups, lanes), i32),
        vm((MOST * rows, lanes), i32),
        vm((length // SLC, rows, QB), f32),
        vm((MOST * rows, QB), f32),
        vm((n, 2, count, width), bf16),
        vm((n, 8, width), f32),
        vm((n, MOST * SLC, width), bf16),
        vm((n, MOST * SLC, width), bf16),
        vm((n, MOST * SLC, width), bf16),
        vm((n, MOST * SLC, width), bf16),
        vm((length, length), f32),
        vm((heads, 1, length), f32),
        vm((heads, 1, length), f32),
        vm((heads, DH, length), f32),
        vm((heads, 1, length), f32),
        vm((heads, DH, length), f32),
        dma((n,)), dma((n,)), dma((n,)), dma((n,)), dma((n,)), dma((n,)),
        dma((n,)), dma((n,)), dma((n,)), dma((n,)),
    ]
    return pl.pallas_call(
        functools.partial(kernel, n),
        out_shape=jax.ShapeDtypeStruct(queries.shape, bf16),
        in_specs=[pl.BlockSpec(memory_space=pltpu.VMEM)] * 10,
        out_specs=pl.BlockSpec(memory_space=pltpu.VMEM),
        scratch_shapes=scratch,
        compiler_params=pltpu.CompilerParams(
            collective_id=0, has_side_effects=True, vmem_limit_bytes=48 << 20
        ),
    )(queries, keys, values, gates, chosen, pool_k, pool_v, out_gain[None], cosine, sine)


def solution(mesh):
    in_specs = (
        P(("grp", "dp"), "kv", "tp"),
        P(("grp", "dp"), "kv", "tp"),
        P(("grp", "dp"), "kv", "tp"),
        P(("grp", "dp"), None, "kv", "tp"),
        P(("grp", "dp"), "kv", "tp", None),
        P(),
        P(),
        P("tp"),
    )
    out_specs = P(("grp", "dp"), "kv", "tp")
    return jax.shard_map(
        per_device, mesh=mesh, in_specs=in_specs, out_specs=out_specs, check_vma=False
    )
```

```python
import functools

import jax
import jax.numpy as jnp
from jax import lax
from jax.experimental import pallas as pl
from jax.experimental.pallas import tpu as pltpu
from jax.sharding import PartitionSpec as P

DH = 64
CMP_STRIDE = 16
CMP_BLOCK = 32
SLC = 64
QB = 128
MOST = 2
THETA = 500000.0
EPS = 1e-06
NEG = -1e30
LOG2E = 1.4426950408889634
MESH = pl.DeviceIdType.MESH


def rope_table(start, length):
    half = DH // 2
    lane = jnp.arange(2 * DH)
    freq = jnp.power(jnp.float32(THETA), -(2.0 * (lane % half).astype(jnp.float32)) / DH)
    angle = (start + jnp.arange(length)).astype(jnp.float32)[:, None] * freq[None, :]
    sign = jnp.where(lane % DH < half, -1.0, 1.0).astype(jnp.float32)
    return jnp.cos(angle), jnp.sin(angle) * sign[None, :]


def turn(x, cosine, sine):
    half = DH // 2
    lane = lax.broadcasted_iota(jnp.int32, x.shape, 1)
    partner = jnp.where(lane % DH < half, pltpu.roll(x, 2 * DH - half, 1), pltpu.roll(x, half, 1))
    return (x * cosine + partner * sine).astype(jnp.bfloat16)


def kernel(
    n, q_ref, k_ref, v_ref, gate_ref, list_ref, pk_ref, pv_ref, gain_ref, cos_ref, sin_ref,
    out_ref,
    qt, kt, vtl, kk, kkr, vtr, skk, svt, req, reqbuf, flag, own_bias, far_bias,
    sumbuf, edge, sendk, sendv, recvk, recvv, bias,
    top, total, acc, stot, sacc,
    req_send, req_recv, sum_send, sum_recv, edge_send, edge_recv,
    k_send, k_recv, v_send, v_recv,
):
    me = lax.axis_index("kv")
    length = q_ref.shape[1]
    heads = q_ref.shape[2] // DH
    groups = k_ref.shape[2] // DH
    per_group = heads // groups
    pairs = per_group // 2
    slabs = groups // 2
    qblocks = length // QB
    per = length // SLC
    count = length // CMP_STRIDE
    scale = DH ** (-0.5) * LOG2E
    f32 = jnp.float32

    barrier = pltpu.get_barrier_semaphore()
    for d in range(1, n):
        pl.semaphore_signal(
            barrier, inc=1, device_id={"kv": lax.rem(me + d, n)}, device_id_type=MESH
        )

    lanes = req.shape[1]
    rows = qblocks * groups

    def column(x, at):
        spot = lax.broadcasted_iota(jnp.int32, x.shape, 1) == at
        picked = jnp.sum(jnp.where(spot, x.astype(f32), 0.0), 1, keepdims=True)
        return jnp.broadcast_to(picked, (x.shape[0], QB))

    lists = jnp.concatenate([list_ref[0, b] for b in range(qblocks)], 0)
    lane = lax.broadcasted_iota(jnp.int32, (rows, lanes), 1)
    member = jnp.zeros((rows, lanes), jnp.int32)
    for i in range(lists.shape[1]):
        member = jnp.where(lists[:, i : i + 1] == lane, 1, member)
    union = member[:groups]
    for b in range(1, qblocks):
        union = jnp.maximum(union, member[b * groups : (b + 1) * groups])
    union = jnp.concatenate([union] * qblocks, 0)
    inner = lane % per
    rank = jnp.zeros_like(union)
    for d in range(1, per):
        rank = rank + jnp.where(inner >= d, pltpu.roll(union, d, 1), 0)

    def first_of(x):
        found = x
        for d in range(1, per):
            found = found + pltpu.roll(x, lanes - d, 1)
        return found

    for j in range(MOST):
        hit = (union == 1) & (rank == j)
        asked = first_of(jnp.where(hit, inner, 0))
        req[j * groups : (j + 1) * groups, :] = asked[:groups]
        flag[j * rows : (j + 1) * rows, :] = first_of(jnp.where(hit, member, 0))
    for i in range(per):
        own_bias[i] = jnp.where(column(member, me * per + i) > 0.5, 0.0, NEG)

    pl.semaphore_wait(barrier, n - 1)

    def remote(src, dst, send, recv, peer, origin):
        return pltpu.make_async_remote_copy(
            src_ref=src, dst_ref=dst, send_sem=send.at[peer], recv_sem=recv.at[origin],
            device_id={"kv": peer}, device_id_type=MESH,
        )

    def ask(peer, origin):
        return remote(req, reqbuf.at[origin], req_send, req_recv, peer, origin)

    def give_sum(peer, origin):
        return remote(sumbuf.at[origin], sumbuf.at[origin], sum_send, sum_recv, peer, origin)

    def give_edge(peer, origin):
        return remote(edge.at[origin], edge.at[origin], edge_send, edge_recv, peer, origin)

    def give_k(peer, origin):
        return remote(sendk.at[peer], recvk.at[origin], k_send, k_recv, peer, origin)

    def give_v(peer, origin):
        return remote(sendv.at[peer], recvv.at[origin], v_send, v_recv, peer, origin)

    @pl.loop(0, me)
    def _(d):
        ask(me - 1 - d, me).start()

    cosine = cos_ref[...]
    sine = sin_ref[...]
    low = lax.broadcasted_iota(jnp.int32, (length, 2 * DH), 1) < DH
    for p in range(slabs):
        cols = slice(p * 2 * DH, (p + 1) * 2 * DH)
        turned = turn(k_ref[0, :, cols].astype(f32), cosine, sine)
        kt[:, cols] = turned
    row = lax.broadcasted_iota(jnp.int32, (count, 2 * DH), 0)
    for w, (src, pool_ref) in enumerate(((k_ref, pk_ref), (v_ref, pv_ref))):
        pool = pool_ref[...]
        pool = jnp.concatenate([pool, pool], 1)
        for p in range(slabs):
            cols = slice(p * 2 * DH, (p + 1) * 2 * DH)
            x = src[0, :, cols].astype(f32).reshape(count, CMP_STRIDE, 2 * DH)
            lower = jnp.sum(x * pool[None, :CMP_STRIDE], 1)
            upper = jnp.sum(x * pool[None, CMP_STRIDE:], 1)
            following = jnp.where(row == count - 1, 0.0, pltpu.roll(upper, count - 1, 0))
            sumbuf[me, w, :, cols] = (lower + following).astype(jnp.bfloat16)
            edge[me, 2 * w : 2 * w + 1, cols] = lower[count - 1 :]
            edge[me, 2 * w + 1 : 2 * w + 2, cols] = upper[:1]

    @pl.loop(me + 1, n)
    def _(r):
        give_sum(r, me).start()
        give_edge(r, me).start()

    low_slc = lax.broadcasted_iota(jnp.int32, (SLC, 2 * DH), 1) < DH

    odd = lax.rem(me, 2)

    @pl.loop(0, n - 1 - me)
    def _(d):
        r = odd * (me + 1 + d) + (1 - odd) * (n - 1 - d)
        ask(me, r).wait_recv()
        ids = column(reqbuf[r], me * per)
        for j in range(MOST):
            place = slice(j * SLC, (j + 1) * SLC)
            for p in range(slabs):
                cols = slice(p * 2 * DH, (p + 1) * 2 * DH)
                at = j * groups + 2 * p
                pick = jnp.where(low_slc, ids[at : at + 1], ids[at + 1 : at + 2])
                k_block = kt[:SLC, cols].astype(f32)
                v_block = v_ref[0, :SLC, cols].astype(f32)
                for i in range(1, per):
                    span = slice(i * SLC, (i + 1) * SLC)
                    match = pick > i - 0.5
                    k_block = jnp.where(match, kt[span, cols].astype(f32), k_block)
                    v_block = jnp.where(match, v_ref[0, span, cols].astype(f32), v_block)
                sendk[r, place, cols] = k_block.astype(jnp.bfloat16)
                sendv[r, place, cols] = v_block.astype(jnp.bfloat16)
        give_k(r, me).start()
        give_v(r, me).start()

    for p in range(heads // 2):
        qt[p] = turn(q_ref[0, :, p * 2 * DH : (p + 1) * 2 * DH].astype(f32), cosine, sine)

    def spread(slab, g, dst):
        keep = lax.broadcasted_iota(jnp.int32, slab.shape, 1) < DH
        wide = slab.astype(f32)
        swapped = pltpu.roll(wide, DH, 1)
        first, second = (wide, swapped) if g % 2 == 0 else (swapped, wide)
        dst[g, 0] = jnp.where(keep, first, 0.0).astype(jnp.bfloat16)
        dst[g, 1] = jnp.where(keep, 0.0, second).astype(jnp.bfloat16)

    def transposed(slab):
        return slab.astype(f32).T.astype(jnp.bfloat16)

    def score(keys, queries):
        return lax.dot_general(
            keys, queries, (((1,), (1,)), ((), ())), preferred_element_type=f32
        )

    for g in range(groups):
        spread(kt[:, (g // 2) * 2 * DH : (g // 2 + 1) * 2 * DH], g, kk)
    for p in range(slabs):
        flip = transposed(v_ref[0, :, p * 2 * DH : (p + 1) * 2 * DH])
        vtl[2 * p] = flip[:DH]
        vtl[2 * p + 1] = flip[DH:]
    key_at = lax.broadcasted_iota(jnp.int32, (SLC, QB), 0)
    token_at = lax.broadcasted_iota(jnp.int32, (SLC, QB), 1)

    @pl.loop(0, groups, unroll=2)
    def _(g):
        for b in range(qblocks):
            for i in range(per):
                value = own_bias[i, pl.ds(b * groups + g, 1), :]
                tile = jnp.where(key_at + i * SLC <= token_at + b * QB, value, NEG)
                bias[i * SLC : (i + 1) * SLC, b * QB : (b + 1) * QB] = tile
        both = kk[g].reshape(2 * length, 2 * DH)
        allowed = bias[...]
        raw = [score(both, qt[g * pairs + pair]) * scale for pair in range(pairs)]
        parts = [
            r[e * length : (e + 1) * length] + allowed for r in raw for e in range(2)
        ]
        tops = [jnp.max(x, 0, keepdims=True) for x in parts]
        weights = [jnp.exp2(x - m) for x, m in zip(parts, tops)]
        totals = [jnp.sum(w, 0, keepdims=True) for w in weights]
        flat = vtl[g]
        sums = [
            jnp.dot(flat, w.astype(jnp.bfloat16), preferred_element_type=f32) for w in weights
        ]
        for o in range(per_group):
            h = g * per_group + o
            top[h] = tops[o]
            total[h] = totals[o]
            acc[h] = sums[o]

    @pl.loop(0, me)
    def _(d):
        give_sum(me, me - 1 - d).wait_recv()
        give_edge(me, me - 1 - d).wait_recv()

    for s in range(n):
        for w in range(2):
            place = slice(s * count, (s + 1) * count)
            for p in range(slabs):
                cols = slice(p * 2 * DH, (p + 1) * 2 * DH)
                following = edge[min(s + 1, n - 1), 2 * w + 1 : 2 * w + 2, cols]
                last = edge[s, 2 * w : 2 * w + 1, cols] + following
                own = sumbuf[s, w, :, cols].astype(f32)
                joined = jnp.where((row == count - 1) & (s < me), last, own)
                joined = jnp.where(s <= me, joined, 0.0)
                if w == 0:
                    for o in range(2):
                        lanes_low = lax.broadcasted_iota(jnp.int32, joined.shape, 1) < DH
                        swapped = pltpu.roll(joined, DH, 1)
                        first, second = (joined, swapped) if o == 0 else (swapped, joined)
                        skk[2 * p + o, 0, place] = jnp.where(lanes_low, first, 0.0).astype(
                            jnp.bfloat16
                        )
                        skk[2 * p + o, 1, place] = jnp.where(lanes_low, 0.0, second).astype(
                            jnp.bfloat16
                        )
                else:
                    svt[place, cols] = joined.astype(jnp.bfloat16)
    part_at = lax.broadcasted_iota(jnp.int32, (n * count, length), 0)
    time_at = lax.broadcasted_iota(jnp.int32, (n * count, length), 1) + me * length
    seen = part_at * CMP_STRIDE + CMP_BLOCK - 1 <= time_at
    sbias = jnp.where(seen, 0.0, NEG)
    flips = [transposed(svt[:, p * 2 * DH : (p + 1) * 2 * DH]) for p in range(slabs)]
    for g in range(groups):
        vt = flips[g // 2][(g % 2) * DH : (g % 2 + 1) * DH]
        both = skk[g].reshape(2 * n * count, 2 * DH)
        raw = [
            score(both, q_ref[0, :, (g * pairs + pair) * 2 * DH : (g * pairs + pair + 1) * 2 * DH])
            * scale
            for pair in range(pairs)
        ]
        parts = [
            r[e * n * count : (e + 1) * n * count] + sbias for r in raw for e in range(2)
        ]
        tops = [jnp.maximum(jnp.max(x, 0, keepdims=True), 0.1 * NEG) for x in parts]
        weights = [jnp.exp2(x - m) for x, m in zip(parts, tops)]
        totals = [jnp.sum(w, 0, keepdims=True) for w in weights]
        sums = [jnp.dot(vt, w.astype(jnp.bfloat16), preferred_element_type=f32) for w in weights]
        for o in range(per_group):
            stot[g * per_group + o] = totals[o]
            sacc[g * per_group + o] = sums[o]

    @pl.loop(0, me)
    def _(d):
        s = lax.rem(me - 1 + d, me)
        give_k(me, s).wait_recv()
        give_v(me, s).wait_recv()
        far_bias[...] = jnp.where(column(flag[...], s * per) > 0.5, 0.0, NEG)
        for g in range(groups):
            spread(recvk[s, :, (g // 2) * 2 * DH : (g // 2 + 1) * 2 * DH], g, kkr)
        for p in range(slabs):
            flip = transposed(recvv[s, :, p * 2 * DH : (p + 1) * 2 * DH])
            vtr[2 * p] = flip[:DH]
            vtr[2 * p + 1] = flip[DH:]

        @pl.loop(0, groups, unroll=4)
        def _(g):
            rowed = [
                jnp.concatenate(
                    [
                        far_bias[pl.ds((j * qblocks + b) * groups + g, 1), :]
                        for b in range(qblocks)
                    ],
                    1,
                )
                for j in range(MOST)
            ]
            size = MOST * SLC
            both = kkr[g].reshape(2 * size, 2 * DH)
            base = g * per_group
            old = [top[base + o] for o in range(per_group)]
            old_total = [total[base + o] for o in range(per_group)]
            old_acc = [acc[base + o] for o in range(per_group)]
            raw = [score(both, qt[g * pairs + pair]) * scale for pair in range(pairs)]
            parts = [
                jnp.concatenate(
                    [
                        r[e * size + j * SLC : e * size + (j + 1) * SLC] + rowed[j]
                        for j in range(MOST)
                    ],
                    0,
                )
                for r in raw
                for e in range(2)
            ]
            tops = [jnp.maximum(jnp.max(x, 0, keepdims=True), m) for x, m in zip(parts, old)]
            weights = [jnp.exp2(x - m) for x, m in zip(parts, tops)]
            shrink = [jnp.exp2(a - m) for a, m in zip(old, tops)]
            totals = [
                t * c + jnp.sum(w, 0, keepdims=True)
                for t, c, w in zip(old_total, shrink, weights)
            ]
            flat = vtr[g]
            sums = [
                a * c + jnp.dot(flat, w.astype(jnp.bfloat16), preferred_element_type=f32)
                for a, c, w in zip(old_acc, shrink, weights)
            ]
            for o in range(per_group):
                top[base + o] = tops[o]
                total[base + o] = totals[o]
                acc[base + o] = sums[o]

    for pair in range(heads // 2):
        both = []
        for e in range(2):
            h = 2 * pair + e
            first, second = (
                1.0 / (1.0 + jnp.exp(-gate_ref[0, w, h : h + 1])) for w in range(2)
            )
            mixed = sacc[h] * (first / jnp.maximum(stot[h], 1.0)) + acc[h] * (
                second / total[h]
            )
            mean = jnp.sum(mixed * mixed, 0, keepdims=True) * (1.0 / DH)
            both.append(mixed * lax.rsqrt(mean + EPS))
        cols = slice(pair * 2 * DH, (pair + 1) * 2 * DH)
        flat = jnp.concatenate(both, 0).T
        out_ref[0, :, cols] = (flat * gain_ref[:, cols]).astype(jnp.bfloat16)

    @pl.loop(0, me)
    def _(d):
        ask(me - 1 - d, me).wait_send()

    @pl.loop(me + 1, n)
    def _(r):
        give_sum(r, me).wait_send()
        give_edge(r, me).wait_send()
        give_k(r, me).wait_send()
        give_v(r, me).wait_send()


def per_device(queries, keys, values, gate_logits, chosen, pool_k, pool_v, out_gain):
    n = lax.axis_size("kv")
    length = queries.shape[1]
    groups = keys.shape[2] // DH
    heads = queries.shape[2] // DH
    qblocks = length // QB
    count = length // CMP_STRIDE
    total = n * (length // SLC)
    lanes = -(-total // 128) * 128
    rows = qblocks * groups
    width = groups * DH
    cosine, sine = rope_table(lax.axis_index("kv") * length, length)
    gates = gate_logits.transpose(0, 1, 3, 2)
    bf16, f32, i32 = jnp.bfloat16, jnp.float32, jnp.int32
    vm, dma = pltpu.VMEM, pltpu.SemaphoreType.DMA
    scratch = [
        vm((heads // 2, length, 2 * DH), bf16),
        vm((length, width), bf16),
        vm((groups, DH, length), bf16),
        vm((groups, 2, length, 2 * DH), bf16),
        vm((groups, 2, MOST * SLC, 2 * DH), bf16),
        vm((groups, DH, MOST * SLC), bf16),
        vm((groups, 2, n * count, 2 * DH), bf16),
        vm((n * count, width), bf16),
        vm((MOST * groups, lanes), i32),
        vm((n, MOST * groups, lanes), i32),
        vm((MOST * rows, lanes), i32),
        vm((length // SLC, rows, QB), f32),
        vm((MOST * rows, QB), f32),
        vm((n, 2, count, width), bf16),
        vm((n, 8, width), f32),
        vm((n, MOST * SLC, width), bf16),
        vm((n, MOST * SLC, width), bf16),
        vm((n, MOST * SLC, width), bf16),
        vm((n, MOST * SLC, width), bf16),
        vm((length, length), f32),
        vm((heads, 1, length), f32),
        vm((heads, 1, length), f32),
        vm((heads, DH, length), f32),
        vm((heads, 1, length), f32),
        vm((heads, DH, length), f32),
        dma((n,)), dma((n,)), dma((n,)), dma((n,)), dma((n,)), dma((n,)),
        dma((n,)), dma((n,)), dma((n,)), dma((n,)),
    ]
    return pl.pallas_call(
        functools.partial(kernel, n),
        out_shape=jax.ShapeDtypeStruct(queries.shape, bf16),
        in_specs=[pl.BlockSpec(memory_space=pltpu.VMEM)] * 10,
        out_specs=pl.BlockSpec(memory_space=pltpu.VMEM),
        scratch_shapes=scratch,
        compiler_params=pltpu.CompilerParams(
            collective_id=0, has_side_effects=True, vmem_limit_bytes=48 << 20
        ),
    )(queries, keys, values, gates, chosen, pool_k, pool_v, out_gain[None], cosine, sine)


def solution(mesh):
    in_specs = (
        P(("grp", "dp"), "kv", "tp"),
        P(("grp", "dp"), "kv", "tp"),
        P(("grp", "dp"), "kv", "tp"),
        P(("grp", "dp"), None, "kv", "tp"),
        P(("grp", "dp"), "kv", "tp", None),
        P(),
        P(),
        P("tp"),
    )
    out_specs = P(("grp", "dp"), "kv", "tp")
    return jax.shard_map(
        per_device, mesh=mesh, in_specs=in_specs, out_specs=out_specs, check_vma=False
    )
```

```python
import functools

import jax
import jax.numpy as jnp
import numpy as np
from jax import lax
from jax.experimental import pallas as pl
from jax.experimental.pallas import tpu as pltpu
from jax.sharding import PartitionSpec as P

DH = 64
CMP_STRIDE = 16
CMP_BLOCK = 32
SLC = 64
QB = 128
MOST = 2
THETA = 500000.0
EPS = 1e-06
NEG = -1e30
LOG2E = 1.4426950408889634
MESH = pl.DeviceIdType.MESH


def frequencies():
    half = DH // 2
    freq = np.power(np.float64(THETA), -(2.0 * (np.arange(2 * DH) % half)) / DH)
    return np.broadcast_to(freq.astype(np.float32), (8, 2 * DH))


def turn(x, cosine, sine):
    half = DH // 2
    lane = lax.broadcasted_iota(jnp.int32, x.shape, 1)
    partner = jnp.where(lane % DH < half, pltpu.roll(x, 2 * DH - half, 1), pltpu.roll(x, half, 1))
    return (x * cosine + partner * sine).astype(jnp.bfloat16)


def kernel(
    n, q_ref, k_ref, v_ref, gate_ref, list_ref, pk_ref, pv_ref, gain_ref, freq_ref,
    out_ref,
    table, qt, kt, vtl, kk, kkr, vtr, skk, svt, req, reqbuf, flag, own_bias, far_bias,
    sumbuf, edge, sendk, sendv, recvk, recvv, bias,
    top, total, acc, stot, sacc,
    req_send, req_recv, sum_send, sum_recv, edge_send, edge_recv,
    k_send, k_recv, v_send, v_recv,
):
    me = lax.axis_index("kv")
    length = q_ref.shape[1]
    heads = q_ref.shape[2] // DH
    groups = k_ref.shape[2] // DH
    per_group = heads // groups
    pairs = per_group // 2
    slabs = groups // 2
    qblocks = length // QB
    per = length // SLC
    count = length // CMP_STRIDE
    scale = DH ** (-0.5) * LOG2E
    f32 = jnp.float32

    barrier = pltpu.get_barrier_semaphore()
    for d in range(1, n):
        pl.semaphore_signal(
            barrier, inc=1, device_id={"kv": lax.rem(me + d, n)}, device_id_type=MESH
        )

    lanes = req.shape[1]
    rows = qblocks * groups

    def column(x, at):
        spot = lax.broadcasted_iota(jnp.int32, x.shape, 1) == at
        picked = jnp.sum(jnp.where(spot, x.astype(f32), 0.0), 1, keepdims=True)
        return jnp.broadcast_to(picked, (x.shape[0], QB))

    lists = jnp.concatenate([list_ref[0, b] for b in range(qblocks)], 0)
    lane = lax.broadcasted_iota(jnp.int32, (rows, lanes), 1)
    member = jnp.zeros((rows, lanes), jnp.int32)
    for i in range(lists.shape[1]):
        member = jnp.where(lists[:, i : i + 1] == lane, 1, member)
    union = member[:groups]
    for b in range(1, qblocks):
        union = jnp.maximum(union, member[b * groups : (b + 1) * groups])
    union = jnp.concatenate([union] * qblocks, 0)
    inner = lane % per
    rank = jnp.zeros_like(union)
    for d in range(1, per):
        rank = rank + jnp.where(inner >= d, pltpu.roll(union, d, 1), 0)

    def first_of(x):
        found = x
        for d in range(1, per):
            found = found + pltpu.roll(x, lanes - d, 1)
        return found

    for j in range(MOST):
        hit = (union == 1) & (rank == j)
        asked = first_of(jnp.where(hit, inner, 0))
        req[j * groups : (j + 1) * groups, :] = asked[:groups]
        flag[j * rows : (j + 1) * rows, :] = first_of(jnp.where(hit, member, 0))
    for i in range(per):
        own_bias[i] = jnp.where(column(member, me * per + i) > 0.5, 0.0, NEG)

    half = DH // 2
    place = lax.broadcasted_iota(jnp.int32, (length, 2 * DH), 0) + me * length
    angle = place.astype(f32) * freq_ref[:1]
    sign = jnp.where(lax.broadcasted_iota(jnp.int32, (1, 2 * DH), 1) % DH < half, -1.0, 1.0)
    table[0] = jnp.cos(angle)
    table[1] = jnp.sin(angle) * sign

    pl.semaphore_wait(barrier, n - 1)

    def remote(src, dst, send, recv, peer, origin):
        return pltpu.make_async_remote_copy(
            src_ref=src, dst_ref=dst, send_sem=send.at[peer], recv_sem=recv.at[origin],
            device_id={"kv": peer}, device_id_type=MESH,
        )

    def ask(peer, origin):
        return remote(req, reqbuf.at[origin], req_send, req_recv, peer, origin)

    def give_sum(peer, origin):
        return remote(sumbuf.at[origin], sumbuf.at[origin], sum_send, sum_recv, peer, origin)

    def give_edge(peer, origin):
        return remote(edge.at[origin], edge.at[origin], edge_send, edge_recv, peer, origin)

    def give_k(peer, origin):
        return remote(sendk.at[peer], recvk.at[origin], k_send, k_recv, peer, origin)

    def give_v(peer, origin):
        return remote(sendv.at[peer], recvv.at[origin], v_send, v_recv, peer, origin)

    @pl.loop(0, me)
    def _(d):
        ask(me - 1 - d, me).start()

    cosine = table[0]
    sine = table[1]
    low = lax.broadcasted_iota(jnp.int32, (length, 2 * DH), 1) < DH
    for p in range(slabs):
        cols = slice(p * 2 * DH, (p + 1) * 2 * DH)
        turned = turn(k_ref[0, :, cols].astype(f32), cosine, sine)
        kt[:, cols] = turned
    row = lax.broadcasted_iota(jnp.int32, (count, 2 * DH), 0)
    for w, (src, pool_ref) in enumerate(((k_ref, pk_ref), (v_ref, pv_ref))):
        pool = pool_ref[...]
        pool = jnp.concatenate([pool, pool], 1)
        for p in range(slabs):
            cols = slice(p * 2 * DH, (p + 1) * 2 * DH)
            x = src[0, :, cols].astype(f32).reshape(count, CMP_STRIDE, 2 * DH)
            lower = jnp.sum(x * pool[None, :CMP_STRIDE], 1)
            upper = jnp.sum(x * pool[None, CMP_STRIDE:], 1)
            following = jnp.where(row == count - 1, 0.0, pltpu.roll(upper, count - 1, 0))
            sumbuf[me, w, :, cols] = (lower + following).astype(jnp.bfloat16)
            edge[me, 2 * w : 2 * w + 1, cols] = lower[count - 1 :]
            edge[me, 2 * w + 1 : 2 * w + 2, cols] = upper[:1]

    @pl.loop(me + 1, n)
    def _(r):
        give_sum(r, me).start()
        give_edge(r, me).start()

    low_slc = lax.broadcasted_iota(jnp.int32, (SLC, 2 * DH), 1) < DH

    odd = lax.rem(me, 2)

    @pl.loop(0, n - 1 - me)
    def _(d):
        r = odd * (me + 1 + d) + (1 - odd) * (n - 1 - d)
        ask(me, r).wait_recv()
        ids = column(reqbuf[r], me * per)
        for j in range(MOST):
            place = slice(j * SLC, (j + 1) * SLC)
            for p in range(slabs):
                cols = slice(p * 2 * DH, (p + 1) * 2 * DH)
                at = j * groups + 2 * p
                pick = jnp.where(low_slc, ids[at : at + 1], ids[at + 1 : at + 2])
                k_block = kt[:SLC, cols].astype(f32)
                v_block = v_ref[0, :SLC, cols].astype(f32)
                for i in range(1, per):
                    span = slice(i * SLC, (i + 1) * SLC)
                    match = pick > i - 0.5
                    k_block = jnp.where(match, kt[span, cols].astype(f32), k_block)
                    v_block = jnp.where(match, v_ref[0, span, cols].astype(f32), v_block)
                sendk[r, place, cols] = k_block.astype(jnp.bfloat16)
                sendv[r, place, cols] = v_block.astype(jnp.bfloat16)
        give_k(r, me).start()
        give_v(r, me).start()

    for p in range(heads // 2):
        qt[p] = turn(q_ref[0, :, p * 2 * DH : (p + 1) * 2 * DH].astype(f32), cosine, sine)

    def spread(slab, g, dst):
        keep = lax.broadcasted_iota(jnp.int32, slab.shape, 1) < DH
        wide = slab.astype(f32)
        swapped = pltpu.roll(wide, DH, 1)
        first, second = (wide, swapped) if g % 2 == 0 else (swapped, wide)
        dst[g, 0] = jnp.where(keep, first, 0.0).astype(jnp.bfloat16)
        dst[g, 1] = jnp.where(keep, 0.0, second).astype(jnp.bfloat16)

    def transposed(slab):
        return slab.astype(f32).T.astype(jnp.bfloat16)

    def score(keys, queries):
        return lax.dot_general(
            keys, queries, (((1,), (1,)), ((), ())), preferred_element_type=f32
        )

    for g in range(groups):
        spread(kt[:, (g // 2) * 2 * DH : (g // 2 + 1) * 2 * DH], g, kk)
    for p in range(slabs):
        flip = transposed(v_ref[0, :, p * 2 * DH : (p + 1) * 2 * DH])
        vtl[2 * p] = flip[:DH]
        vtl[2 * p + 1] = flip[DH:]
    key_at = lax.broadcasted_iota(jnp.int32, (SLC, QB), 0)
    token_at = lax.broadcasted_iota(jnp.int32, (SLC, QB), 1)

    @pl.loop(0, groups, unroll=2)
    def _(g):
        for b in range(qblocks):
            for i in range(per):
                value = own_bias[i, pl.ds(b * groups + g, 1), :]
                tile = jnp.where(key_at + i * SLC <= token_at + b * QB, value, NEG)
                bias[i * SLC : (i + 1) * SLC, b * QB : (b + 1) * QB] = tile
        both = kk[g].reshape(2 * length, 2 * DH)
        allowed = bias[...]
        raw = [score(both, qt[g * pairs + pair]) * scale for pair in range(pairs)]
        parts = [
            r[e * length : (e + 1) * length] + allowed for r in raw for e in range(2)
        ]
        tops = [jnp.max(x, 0, keepdims=True) for x in parts]
        weights = [jnp.exp2(x - m) for x, m in zip(parts, tops)]
        totals = [jnp.sum(w, 0, keepdims=True) for w in weights]
        flat = vtl[g]
        sums = [
            jnp.dot(flat, w.astype(jnp.bfloat16), preferred_element_type=f32) for w in weights
        ]
        for o in range(per_group):
            h = g * per_group + o
            top[h] = tops[o]
            total[h] = totals[o]
            acc[h] = sums[o]

    @pl.loop(0, me)
    def _(d):
        give_sum(me, me - 1 - d).wait_recv()
        give_edge(me, me - 1 - d).wait_recv()

    for s in range(n):
        for w in range(2):
            place = slice(s * count, (s + 1) * count)
            for p in range(slabs):
                cols = slice(p * 2 * DH, (p + 1) * 2 * DH)
                following = edge[min(s + 1, n - 1), 2 * w + 1 : 2 * w + 2, cols]
                last = edge[s, 2 * w : 2 * w + 1, cols] + following
                own = sumbuf[s, w, :, cols].astype(f32)
                joined = jnp.where((row == count - 1) & (s < me), last, own)
                joined = jnp.where(s <= me, joined, 0.0)
                if w == 0:
                    for o in range(2):
                        lanes_low = lax.broadcasted_iota(jnp.int32, joined.shape, 1) < DH
                        swapped = pltpu.roll(joined, DH, 1)
                        first, second = (joined, swapped) if o == 0 else (swapped, joined)
                        skk[2 * p + o, 0, place] = jnp.where(lanes_low, first, 0.0).astype(
                            jnp.bfloat16
                        )
                        skk[2 * p + o, 1, place] = jnp.where(lanes_low, 0.0, second).astype(
                            jnp.bfloat16
                        )
                else:
                    svt[place, cols] = joined.astype(jnp.bfloat16)
    part_at = lax.broadcasted_iota(jnp.int32, (n * count, length), 0)
    time_at = lax.broadcasted_iota(jnp.int32, (n * count, length), 1) + me * length
    seen = part_at * CMP_STRIDE + CMP_BLOCK - 1 <= time_at
    sbias = jnp.where(seen, 0.0, NEG)
    flips = [transposed(svt[:, p * 2 * DH : (p + 1) * 2 * DH]) for p in range(slabs)]
    for g in range(groups):
        vt = flips[g // 2][(g % 2) * DH : (g % 2 + 1) * DH]
        both = skk[g].reshape(2 * n * count, 2 * DH)
        raw = [
            score(both, q_ref[0, :, (g * pairs + pair) * 2 * DH : (g * pairs + pair + 1) * 2 * DH])
            * scale
            for pair in range(pairs)
        ]
        parts = [
            r[e * n * count : (e + 1) * n * count] + sbias for r in raw for e in range(2)
        ]
        tops = [jnp.maximum(jnp.max(x, 0, keepdims=True), 0.1 * NEG) for x in parts]
        weights = [jnp.exp2(x - m) for x, m in zip(parts, tops)]
        totals = [jnp.sum(w, 0, keepdims=True) for w in weights]
        sums = [jnp.dot(vt, w.astype(jnp.bfloat16), preferred_element_type=f32) for w in weights]
        for o in range(per_group):
            stot[g * per_group + o] = totals[o]
            sacc[g * per_group + o] = sums[o]

    @pl.loop(0, me)
    def _(d):
        s = lax.rem(me - 1 + d, me)
        give_k(me, s).wait_recv()
        give_v(me, s).wait_recv()
        far_bias[...] = jnp.where(column(flag[...], s * per) > 0.5, 0.0, NEG)
        for g in range(groups):
            spread(recvk[s, :, (g // 2) * 2 * DH : (g // 2 + 1) * 2 * DH], g, kkr)
        for p in range(slabs):
            flip = transposed(recvv[s, :, p * 2 * DH : (p + 1) * 2 * DH])
            vtr[2 * p] = flip[:DH]
            vtr[2 * p + 1] = flip[DH:]

        @pl.loop(0, groups, unroll=4)
        def _(g):
            rowed = [
                jnp.concatenate(
                    [
                        far_bias[pl.ds((j * qblocks + b) * groups + g, 1), :]
                        for b in range(qblocks)
                    ],
                    1,
                )
                for j in range(MOST)
            ]
            size = MOST * SLC
            both = kkr[g].reshape(2 * size, 2 * DH)
            base = g * per_group
            old = [top[base + o] for o in range(per_group)]
            old_total = [total[base + o] for o in range(per_group)]
            old_acc = [acc[base + o] for o in range(per_group)]
            raw = [score(both, qt[g * pairs + pair]) * scale for pair in range(pairs)]
            parts = [
                jnp.concatenate(
                    [
                        r[e * size + j * SLC : e * size + (j + 1) * SLC] + rowed[j]
                        for j in range(MOST)
                    ],
                    0,
                )
                for r in raw
                for e in range(2)
            ]
            tops = [jnp.maximum(jnp.max(x, 0, keepdims=True), m) for x, m in zip(parts, old)]
            weights = [jnp.exp2(x - m) for x, m in zip(parts, tops)]
            shrink = [jnp.exp2(a - m) for a, m in zip(old, tops)]
            totals = [
                t * c + jnp.sum(w, 0, keepdims=True)
                for t, c, w in zip(old_total, shrink, weights)
            ]
            flat = vtr[g]
            sums = [
                a * c + jnp.dot(flat, w.astype(jnp.bfloat16), preferred_element_type=f32)
                for a, c, w in zip(old_acc, shrink, weights)
            ]
            for o in range(per_group):
                top[base + o] = tops[o]
                total[base + o] = totals[o]
                acc[base + o] = sums[o]

    for pair in range(heads // 2):
        both = []
        for e in range(2):
            h = 2 * pair + e
            first, second = (
                1.0 / (1.0 + jnp.exp(-gate_ref[0, w, h : h + 1])) for w in range(2)
            )
            mixed = sacc[h] * (first / jnp.maximum(stot[h], 1.0)) + acc[h] * (
                second / total[h]
            )
            mean = jnp.sum(mixed * mixed, 0, keepdims=True) * (1.0 / DH)
            both.append(mixed * lax.rsqrt(mean + EPS))
        cols = slice(pair * 2 * DH, (pair + 1) * 2 * DH)
        flat = jnp.concatenate(both, 0).T
        out_ref[0, :, cols] = (flat * gain_ref[:, cols]).astype(jnp.bfloat16)

    @pl.loop(0, me)
    def _(d):
        ask(me - 1 - d, me).wait_send()

    @pl.loop(me + 1, n)
    def _(r):
        give_sum(r, me).wait_send()
        give_edge(r, me).wait_send()
        give_k(r, me).wait_send()
        give_v(r, me).wait_send()


def per_device(queries, keys, values, gate_logits, chosen, pool_k, pool_v, out_gain):
    n = lax.axis_size("kv")
    length = queries.shape[1]
    groups = keys.shape[2] // DH
    heads = queries.shape[2] // DH
    qblocks = length // QB
    count = length // CMP_STRIDE
    total = n * (length // SLC)
    lanes = -(-total // 128) * 128
    rows = qblocks * groups
    width = groups * DH
    gates = gate_logits.transpose(0, 1, 3, 2)
    bf16, f32, i32 = jnp.bfloat16, jnp.float32, jnp.int32
    vm, dma = pltpu.VMEM, pltpu.SemaphoreType.DMA
    scratch = [
        vm((2, length, 2 * DH), f32),
        vm((heads // 2, length, 2 * DH), bf16),
        vm((length, width), bf16),
        vm((groups, DH, length), bf16),
        vm((groups, 2, length, 2 * DH), bf16),
        vm((groups, 2, MOST * SLC, 2 * DH), bf16),
        vm((groups, DH, MOST * SLC), bf16),
        vm((groups, 2, n * count, 2 * DH), bf16),
        vm((n * count, width), bf16),
        vm((MOST * groups, lanes), i32),
        vm((n, MOST * groups, lanes), i32),
        vm((MOST * rows, lanes), i32),
        vm((length // SLC, rows, QB), f32),
        vm((MOST * rows, QB), f32),
        vm((n, 2, count, width), bf16),
        vm((n, 8, width), f32),
        vm((n, MOST * SLC, width), bf16),
        vm((n, MOST * SLC, width), bf16),
        vm((n, MOST * SLC, width), bf16),
        vm((n, MOST * SLC, width), bf16),
        vm((length, length), f32),
        vm((heads, 1, length), f32),
        vm((heads, 1, length), f32),
        vm((heads, DH, length), f32),
        vm((heads, 1, length), f32),
        vm((heads, DH, length), f32),
        dma((n,)), dma((n,)), dma((n,)), dma((n,)), dma((n,)), dma((n,)),
        dma((n,)), dma((n,)), dma((n,)), dma((n,)),
    ]
    return pl.pallas_call(
        functools.partial(kernel, n),
        out_shape=jax.ShapeDtypeStruct(queries.shape, bf16),
        in_specs=[pl.BlockSpec(memory_space=pltpu.VMEM)] * 9,
        out_specs=pl.BlockSpec(memory_space=pltpu.VMEM),
        scratch_shapes=scratch,
        compiler_params=pltpu.CompilerParams(
            collective_id=0, has_side_effects=True, vmem_limit_bytes=48 << 20
        ),
    )(queries, keys, values, gates, chosen, pool_k, pool_v, out_gain[None], jnp.asarray(frequencies()))


def solution(mesh):
    in_specs = (
        P(("grp", "dp"), "kv", "tp"),
        P(("grp", "dp"), "kv", "tp"),
        P(("grp", "dp"), "kv", "tp"),
        P(("grp", "dp"), None, "kv", "tp"),
        P(("grp", "dp"), "kv", "tp", None),
        P(),
        P(),
        P("tp"),
    )
    out_specs = P(("grp", "dp"), "kv", "tp")
    return jax.shard_map(
        per_device, mesh=mesh, in_specs=in_specs, out_specs=out_specs, check_vma=False
    )
```
